32 devices in a mesh: grp: 2 (over y), sp: 4 (over z), dp: 4 (over x, core).
Axes of the slice: x: 2, y: 2, z: 4, core: 2. Of those that a mesh axis runs over, the one named last changes fastest.
Arguments:
- mixer_source_array: bfloat16 [8, 768, 2048], P(('grp', 'dp'), 'sp'), parts along dimension 0, may hold values from -6 to 6
- source_projection: bfloat16 [2048, 1024], P('dp'), may hold values from -0.125 to 0.125
- gating_projection: bfloat16 [2048, 1024], P('dp'), may hold values from -0.125 to 0.125
- entry_mapping_projection: bfloat16 [2048, 256], replicated, may hold values from -0.0390625 to 0.0390625
- readout_mapping_projection: bfloat16 [2048, 256], replicated, may hold values from -0.0390625 to 0.0390625
- increment_projection: bfloat16 [2048, 16], replicated, may hold values from -0.125 to 0.125
- source_conv_taps: float32 [4, 1024], replicated, may hold values from -3 to 3
- entry_mapping_taps: float32 [4, 256], replicated, may hold values from -3 to 3
- readout_mapping_taps: float32 [4, 256], replicated, may hold values from -3 to 3
- increment_offsets: float32 [16], replicated, may hold values from -1 to 1
- channel_damping_rate: float32 [16], replicated, may hold values from 0 to 1
- bypass_coefficients: float32 [16], replicated, may hold values from 0.5 to 1.5
- stride_multiplier: float32 [8, 768], P(('grp', 'dp')), parts along dimension 0, may hold values from 0.5 to 2
- added_log_damping: float32 [8, 768, 16], P(('grp', 'dp')), parts along dimension 0, may hold values from -2.1 to 0
- norm_scale_factor: float32 [1024], replicated, may hold values from 0.1 to 1.9
- final_projection: bfloat16 [1024, 2048], P(None, 'dp'), may hold values from -0.1875 to 0.1875
Outputs:
- output: bfloat16 [8, 768, 2048], P(('grp', 'dp'), 'sp'), parts along dimension 0
The draws below stay inside these ranges and needn't reach their ends.
There are 2 independent parts, one for each index of `grp`. The reference program is written for one: setup_inputs(seed, part) draws one part's arguments, and reference() takes and returns one part's arrays. A program takes and returns all parts, laid end to end along the dimension named above; an argument that names none is the same for every part. Nothing has to cross between parts.
All inputs are finite; a program needn't handle non-finite values.
Results may differ from the reference program's by a relative error of at most 0.015.
Values may be sent and summed in bfloat16 or wider, within the bound.
A program may use at most 64 MiB of HBM per device.

```python
import math
import jax
import jax.numpy as jnp
from jax import lax

D = 2048
H = 16
P_SIZE = 64
N = 128
G = 2
CONV_W = 4
BLK = 64
TOK_DEV = 192
LEN = 768
SEQS = 4


def draw_channel_damping_rate(key, part):
    base = jax.random.fold_in(key, 101)
    key_kind, key_fast, key_slow = jax.random.split(base, 3)
    fast_share = 0.5
    fast_mask = jax.random.uniform(key_kind, (H,), jnp.float32) < fast_share
    fast_rate = jax.random.uniform(key_fast, (H,), jnp.float32, math.log(1.5 / BLK), math.log(2.5 / BLK))
    slow_rate = jax.random.uniform(key_slow, (H,), jnp.float32, math.log(0.1 / LEN), math.log(0.8 / LEN))
    return jnp.exp(jnp.where(fast_mask, fast_rate, slow_rate))


def draw_stride_multiplier(key, part):
    base = jax.random.fold_in(key, 202)
    shards = LEN // TOK_DEV
    factors = jnp.exp(jax.random.uniform(base, (SEQS, shards), jnp.float32, math.log(0.5), math.log(2.0)))
    return jnp.repeat(factors, TOK_DEV, axis=1)


def draw_added_log_damping(key, part):
    base = jax.random.fold_in(key, 303)
    key_spot, key_loss = jax.random.split(base, 2)
    spots = jax.random.randint(key_spot, (SEQS, 3), 0, LEN)
    losses = jax.random.uniform(key_loss, (SEQS, 3, H), jnp.float32, math.log(0.5), math.log(0.8))
    marks = (jnp.arange(LEN)[None, None, :] == spots[:, :, None]).astype(jnp.float32)
    return jnp.einsum('sbl,sbh->slh', marks, losses)


def steps_of(own_key, dims, pieces, least, top_value):
    factor_of, own = 1.0, jax.random.fold_in(own_key, 6)
    for axis_at, shards_of in pieces:
        heights = jnp.exp(jax.random.uniform(jax.random.fold_in(own, axis_at), (shards_of,), jnp.float32, least / len(pieces), top_value / len(pieces)))
        factor_of = factor_of * jnp.repeat(heights, dims[axis_at] // shards_of).reshape([-1 if axis == axis_at else 1 for axis in range(len(dims))])
    return factor_of


def centred(rng, shape, deviation, reach, pieces=(), kind=jnp.bfloat16):
    gain = steps_of(rng, shape, pieces, -0.22, 0.18) if pieces else 1.0
    drawn = jax.random.normal(rng, shape, jnp.float32) * deviation * gain
    return jnp.minimum(jnp.maximum(drawn, -reach), reach).astype(kind)


def setup_inputs(seed: int = 0, part: int = 0) -> dict:
    key_of = jax.random.split(jax.random.key(seed), 17)
    part_keys = jax.random.split(jax.random.fold_in(key_of[16], part), 17)
    return {
        "mixer_source_array": centred(part_keys[0], (SEQS, LEN, D), 1.0, 6.0, ((0, 4), (1, 4))),
        "source_projection": centred(key_of[1], (D, H * P_SIZE), D ** -0.5, 0.125, ((0, 4),)),
        "gating_projection": centred(key_of[2], (D, H * P_SIZE), D ** -0.5, 0.125, ((0, 4),)),
        "entry_mapping_projection": centred(key_of[3], (D, G * N), (10 * D) ** -0.5, 0.0390625),
        "readout_mapping_projection": centred(key_of[4], (D, G * N), (10 * D) ** -0.5, 0.0390625),
        "increment_projection": centred(key_of[5], (D, H), D ** -0.5, 0.125),
        "source_conv_taps": centred(key_of[6], (CONV_W, H * P_SIZE), CONV_W ** -0.5, 3.0, (), jnp.float32),
        "entry_mapping_taps": centred(key_of[7], (CONV_W, G * N), CONV_W ** -0.5, 3.0, (), jnp.float32),
        "readout_mapping_taps": centred(key_of[8], (CONV_W, G * N), CONV_W ** -0.5, 3.0, (), jnp.float32),
        "increment_offsets": jnp.clip(jax.random.uniform(key_of[9], (H,), jnp.float32, -1.0, 1.0), -1.0, 1.0),
        "channel_damping_rate": draw_channel_damping_rate(jax.random.fold_in(key_of[16], 71), part),
        "bypass_coefficients": jnp.clip(jax.random.uniform(key_of[11], (H,), jnp.float32, 0.5, 1.5), 0.5, 1.5),
        "stride_multiplier": draw_stride_multiplier(jax.random.fold_in(jax.random.fold_in(key_of[16], part), 71), part),
        "added_log_damping": draw_added_log_damping(jax.random.fold_in(jax.random.fold_in(key_of[16], part), 71), part),
        "norm_scale_factor": jnp.clip(1.0 + 0.18 * jax.random.normal(key_of[14], (H * P_SIZE,), jnp.float32), 0.1, 1.9),
        "final_projection": centred(key_of[15], (H * P_SIZE, D), (H * P_SIZE) ** -0.5, 0.1875, ((1, 4),)),
    }


EPSILON = 1e-06
HIGH = lax.Precision.HIGHEST

def conv_silu(padded, taps):
    width = taps.shape[0]
    length = padded.shape[0] - width + 1
    total = taps[0][None, :] * padded[0:length]
    for shift_pos in range(1, width):
        total = total + taps[shift_pos][None, :] * padded[shift_pos:shift_pos + length]
    return jax.nn.silu(total).astype(jnp.bfloat16)

def block_parts(x_blocks, b_blocks, c_blocks, step_width_value, logarithm_retain):
    cumulative = jnp.cumsum(logarithm_retain, axis=1)
    scaled = (x_blocks.astype(jnp.float32) * step_width_value[..., None]).astype(jnp.bfloat16)
    intersection = jnp.einsum('kign,kjgn->kgij', c_blocks.astype(jnp.float32), b_blocks.astype(jnp.float32), precision=HIGH)
    by_row = jnp.transpose(cumulative, (0, 2, 3, 1))
    log_gap = by_row[..., :, None] - by_row[..., None, :]
    length = log_gap.shape[-1]
    lower = jnp.tril(jnp.ones((length, length), bool))
    mixing = (intersection[:, :, None] * jnp.exp(jnp.where(lower, log_gap, -jnp.inf))).astype(jnp.bfloat16)
    inner = jnp.einsum('kgrij,kjgrp->kigrp', mixing.astype(jnp.float32), scaled.astype(jnp.float32), precision=HIGH)
    to_end = jnp.exp(cumulative[:, -1:] - cumulative)
    weighted = (b_blocks[:, :, :, None, :].astype(jnp.float32) * to_end[..., None]).astype(jnp.bfloat16)
    states = jnp.einsum('kjgrn,kjgrp->kgrnp', weighted.astype(jnp.float32), scaled.astype(jnp.float32), precision=HIGH)
    return (inner, states, cumulative[:, -1], cumulative)

def block_carry(states, block_total):
    incl_sum = jnp.cumsum(block_total, axis=0)
    excl_sum = incl_sum - block_total
    count = block_total.shape[0]
    log_gap = excl_sum[:, None] - incl_sum[None, :]
    before = (jnp.arange(count)[None, :] < jnp.arange(count)[:, None])[:, :, None, None]
    factors = jnp.exp(jnp.where(before, log_gap, -jnp.inf))
    carried = jnp.einsum('kjgr,jgrnp->kgrnp', factors, states, precision=HIGH)
    return carried

def block_finish(inner, c_blocks, cumulative, carried, x_blocks, skip):
    reached = jnp.einsum('kign,kgrnp->kigrp', c_blocks.astype(jnp.float32), carried, precision=HIGH)
    return inner + reached * jnp.exp(cumulative)[..., None] + skip[..., None] * x_blocks.astype(jnp.float32)

def reference(mixer_source_array, source_projection, gating_projection, entry_mapping_projection, readout_mapping_projection, increment_projection, source_conv_taps, entry_mapping_taps, readout_mapping_taps, increment_offsets, channel_damping_rate, bypass_coefficients, stride_multiplier, added_log_damping, norm_scale_factor, final_projection):
    per_group = H // G
    blocks = LEN // BLK

    def lone_stream_case(input_rows):
        hidden_width, tempo_row_values, surge_row_values = input_rows
        proj_x = jnp.dot(hidden_width, source_projection, preferred_element_type=jnp.float32).astype(jnp.bfloat16)
        gate_z = jnp.dot(hidden_width, gating_projection, preferred_element_type=jnp.float32).astype(jnp.bfloat16)
        proj_b = jnp.dot(hidden_width, entry_mapping_projection, preferred_element_type=jnp.float32).astype(jnp.bfloat16)
        proj_c = jnp.dot(hidden_width, readout_mapping_projection, preferred_element_type=jnp.float32).astype(jnp.bfloat16)
        step_raw = jnp.dot(hidden_width, increment_projection, preferred_element_type=jnp.float32).astype(jnp.bfloat16)
        xs = conv_silu(jnp.concatenate([jnp.zeros((CONV_W - 1, H * P_SIZE), jnp.float32), proj_x.astype(jnp.float32)], 0), source_conv_taps)
        bm = conv_silu(jnp.concatenate([jnp.zeros((CONV_W - 1, G * N), jnp.float32), proj_b.astype(jnp.float32)], 0), entry_mapping_taps)
        cm = conv_silu(jnp.concatenate([jnp.zeros((CONV_W - 1, G * N), jnp.float32), proj_c.astype(jnp.float32)], 0), readout_mapping_taps)
        step_width_value = jax.nn.softplus(step_raw.astype(jnp.float32) + increment_offsets[None, :])
        logarithm_retain = -channel_damping_rate[None, :] * step_width_value * tempo_row_values[:, None] + surge_row_values
        x_blocks = xs.reshape(blocks, BLK, G, per_group, P_SIZE)
        b_blocks = bm.reshape(blocks, BLK, G, N)
        c_blocks = cm.reshape(blocks, BLK, G, N)
        inner, states, block_total, cumulative = block_parts(x_blocks, b_blocks, c_blocks, step_width_value.reshape(blocks, BLK, G, per_group), logarithm_retain.reshape(blocks, BLK, G, per_group))
        carried = block_carry(states, block_total)
        mixed = block_finish(inner, c_blocks, cumulative, carried, x_blocks, bypass_coefficients.reshape(G, per_group))
        mixed = mixed.astype(jnp.bfloat16).reshape(LEN, H * P_SIZE)
        gated = mixed.astype(jnp.float32) * jax.nn.silu(gate_z.astype(jnp.float32))
        grouped = gated.reshape(LEN, G, H * P_SIZE // G)
        normed = grouped * lax.rsqrt(lax.optimization_barrier(jnp.mean(grouped * grouped, axis=-1, keepdims=True)) + EPSILON)
        normed = (normed.reshape(LEN, H * P_SIZE) * norm_scale_factor[None, :]).astype(jnp.bfloat16)
        return jnp.dot(normed, final_projection, preferred_element_type=jnp.float32).astype(jnp.bfloat16)
    return lax.map(lone_stream_case, (mixer_source_array, stride_multiplier, added_log_damping))
```

```python
import functools

import jax
import jax.numpy as jnp
from jax import lax
from jax.experimental import pallas as pl
from jax.experimental.pallas import tpu as pltpu
from jax.sharding import PartitionSpec as P

P_SIZE = 64
N = 128
G = 2
CONV_W = 4
EPSILON = 1e-06
HIGH = lax.Precision.HIGHEST
MESH = pl.DeviceIdType.MESH
HALO = 16
F32 = jnp.float32
BF16 = jnp.bfloat16


def dot(a, b, dims=((1,), (0,)), precision=None):
    return lax.dot_general(a, b, (dims, ((), ())), precision=precision, preferred_element_type=F32)


def silu(v):
    return v * (1.0 / (1.0 + jnp.exp(-v)))


def kernel(
    dims,
    x_hbm,
    wx_hbm,
    wz_hbm,
    wf_hbm,
    wb_ref,
    wc_ref,
    wdt_ref,
    tx_ref,
    tb_ref,
    tc_ref,
    off_ref,
    rate_ref,
    skip_ref,
    stride_ref,
    damp_ref,
    scale_ref,
    out_ref,
    xe,
    wx,
    wz,
    wf,
    pbc,
    px,
    bm,
    cm,
    xs,
    sc,
    y,
    st,
    car,
    snd,
    nrm,
    loc_sem,
    halo_send,
    halo_recv,
    x_send,
    x_recv,
    y_send,
    y_recv,
    d_send,
    d_recv,
    c_send,
    c_recv,
):
    n_grp, n_sp, n_dp, chunks, c_chunks = dims
    n_x = n_dp // 2
    grp, z, dp = (lax.axis_index(a) for a in ("grp", "sp", "dp"))
    xi, core = dp // 2, dp % 2
    tok = out_ref.shape[0]
    width = xs.shape[1]
    heads = off_ref.shape[1]
    per_group = heads // G
    gw = width // G
    partner = {"dp": xi * 2 + 1 - core}
    y_peer = {"grp": 1 - grp}
    srcs = (wx_hbm, wz_hbm, wf_hbm)

    def at(w, owner, start, rows):
        if w == 2:
            return wf.at[owner, pl.ds(start, rows)]
        ref = (wx, wz)[w]
        return ref.at[pl.ds(pl.multiple_of(owner * srcs[w].shape[0] + start, 16), rows)]

    barrier = pltpu.get_barrier_semaphore()
    peers = [partner, y_peer]
    peers += [{"dp": lax.rem(xi + o, n_x) * 2 + core} for o in range(1, n_x)]
    for peer in peers:
        pl.semaphore_signal(barrier, inc=1, device_id=peer, device_id_type=MESH)

    @pl.when(z > 0)
    def _():
        pl.semaphore_signal(barrier, inc=1, device_id={"sp": z - 1}, device_id_type=MESH)

    @pl.when(z < n_sp - 1)
    def _():
        pl.semaphore_signal(barrier, inc=1, device_id={"sp": z + 1}, device_id_type=MESH)

    x_copy = pltpu.make_async_copy(x_hbm, xe.at[pl.ds(HALO, tok)], loc_sem.at[3])
    x_copy.start()
    own = []
    for w in range(3):
        copy = pltpu.make_async_copy(srcs[w], at(w, dp, 0, srcs[w].shape[0]), loc_sem.at[w])
        copy.start()
        own.append(copy)

    pl.semaphore_wait(barrier, len(peers) + jnp.minimum(z, 1) + jnp.minimum(n_sp - 1 - z, 1))

    def remote(src, dst, send, recv, peer):
        return pltpu.make_async_remote_copy(
            src_ref=src, dst_ref=dst, send_sem=send, recv_sem=recv,
            device_id=peer, device_id_type=MESH,
        )

    def halo_copy():
        return remote(
            x_hbm.at[pl.ds(tok - HALO, HALO)], xe.at[pl.ds(0, HALO)],
            halo_send, halo_recv, {"sp": jnp.minimum(z + 1, n_sp - 1)},
        )

    @pl.when(z < n_sp - 1)
    def _():
        halo_copy().start()

    sends = []

    def x_copy_of(w, o, k, owner, src=None):
        half = srcs[w].shape[0] // n_grp
        rows = half // chunks
        start = grp * half + k * rows
        place = at(w, owner, start, rows)
        if src is not None:
            src = src.at[pl.ds(start, rows)]
        return remote(
            place if src is None else src, place,
            x_send.at[w, o - 1, k], x_recv.at[w, o - 1, k],
            {"dp": lax.rem(xi + o, n_x) * 2 + core},
        )

    for w in range(3):
        for k in range(chunks):
            for o in range(1, n_x):
                copy = x_copy_of(w, o, k, dp, srcs[w])
                copy.start()
                sends.append(copy)
        copy = remote(
            srcs[w], at(w, dp, 0, srcs[w].shape[0]), d_send.at[w, 0], d_recv.at[w], partner
        )
        copy.start()
        sends.append(copy)

    def owner_of(o):
        return lax.rem(xi - o + n_x, n_x) * 2 + core

    def pump(w, k):
        half = srcs[w].shape[0] // n_grp
        rows = half // chunks
        for o in range(1, n_x):
            x_copy_of(w, o, k, owner_of(o)).wait_recv()
            place = at(w, owner_of(o), grp * half + k * rows, rows)
            copy = remote(place, place, y_send.at[w, o - 1, k], y_recv.at[w, o - 1], y_peer)
            copy.start()
            sends.append(copy)
            if k == chunks - 1:
                place = at(w, owner_of(o), grp * half, half)
                copy = remote(place, place, d_send.at[w, o], d_recv.at[w], partner)
                copy.start()
                sends.append(copy)

    def finish(w):
        half = srcs[w].shape[0] // n_grp
        for o in range(1, n_x):
            place = at(w, owner_of(o), (1 - grp) * half, half)
            remote(place, place, y_send.at[w, o - 1, 0], y_recv.at[w, o - 1], y_peer).wait_recv()
            copy = remote(place, place, d_send.at[w, n_x - 1 + o], d_recv.at[w], partner)
            copy.start()
            sends.append(copy)
        own[w].wait()
        if w == 2:
            place = wf.at[pl.ds(0, n_x)]
        else:
            place = (wx, wz)[w].at[pl.ds(0, n_x * srcs[w].shape[0])]
        remote(place, place, d_send.at[w, 0], d_recv.at[w], partner).wait_recv()

    @pl.when(z == 0)
    def _():
        xe[pl.ds(0, HALO), :] = jnp.zeros((HALO, xe.shape[1]), BF16)

    @pl.when(z > 0)
    def _():
        halo_copy().wait_recv()

    x_copy.wait()
    gn = G * N
    pbc[:, 0:gn] = dot(xe[...], wb_ref[...]).astype(BF16).astype(F32)
    pbc[:, gn : 2 * gn] = dot(xe[...], wc_ref[...]).astype(BF16).astype(F32)
    raw = dot(xe[pl.ds(HALO, tok), :], wdt_ref[...]).astype(BF16).astype(F32)

    def conv(buf, cols, taps):
        total = taps[0:1, :] * buf[pl.ds(HALO - CONV_W + 1, tok), cols]
        for k in range(1, CONV_W):
            total = total + taps[k : k + 1, :] * buf[pl.ds(HALO - CONV_W + 1 + k, tok), cols]
        return silu(total).astype(BF16)

    bm[...] = conv(pbc, pl.ds(0, gn), tb_ref[...])
    cm[...] = conv(pbc, pl.ds(gn, gn), tc_ref[...])
    pre = raw + off_ref[...]
    step = jnp.maximum(pre, 0.0) + jnp.log1p(jnp.exp(-jnp.abs(pre)))
    length = stride_ref.shape[1]
    here = lax.broadcasted_iota(jnp.int32, (tok, length), 0) + z * tok
    at_pos = here == lax.broadcasted_iota(jnp.int32, (tok, length), 1)
    tempo = jnp.sum(jnp.where(at_pos, stride_ref[...], 0.0), axis=1, keepdims=True)
    damp = damp_ref[0, pl.ds(pl.multiple_of(z * tok, 8), tok), :]
    keep = -rate_ref[...] * step * tempo + damp
    row = lax.broadcasted_iota(jnp.int32, (tok, tok), 0)
    col = lax.broadcasted_iota(jnp.int32, (tok, tok), 1)
    lower = row >= col
    cum = dot(lower.astype(F32), keep, precision=HIGH)
    cum_t = dot(keep, (row <= col).astype(F32), ((0,), (0,)), HIGH)
    last = cum[tok - 1 : tok, :]
    to_end = jnp.exp(last - cum)
    reach = jnp.exp(cum)
    whole = jnp.exp(last)
    first_head = lax.broadcasted_iota(jnp.int32, (tok, 2 * P_SIZE), 1) < P_SIZE
    first_row = first_head[0:1, :]

    def spread(values, p, mask):
        return jnp.where(mask, values[:, 2 * p : 2 * p + 1], values[:, 2 * p + 1 : 2 * p + 2])

    def pair_cols(p):
        return pl.ds(p * 2 * P_SIZE, 2 * P_SIZE)

    for k in range(chunks):
        pump(0, k)
    finish(0)

    tile = 256

    def project_x(j, carry):
        cols = pl.ds(pl.multiple_of(j * tile, tile), tile)
        px[:, cols] = dot(xe[...], wx[:, cols]).astype(BF16).astype(F32)
        xs[:, cols] = conv(px, cols, tx_ref[:, cols])
        return carry

    lax.fori_loop(0, width // tile, project_x, 0)
    pump(1, 0)

    scaled = []
    for p in range(heads // 2):
        xp = xs[:, pair_cols(p)].astype(F32)
        s = (xp * spread(step, p, first_head)).astype(BF16)
        sc[:, pair_cols(p)] = (s.astype(F32) * spread(to_end, p, first_head)).astype(BF16)
        y[:, pair_cols(p)] = spread(skip_ref[...], p, first_row) * xp
        scaled.append(s)
    for g in range(G):
        cols = pl.ds(g * gw, gw)
        st[:, cols] = dot(bm[:, g * N : (g + 1) * N], sc[:, cols], ((0,), (0,)))

    cw = width // c_chunks

    def chain_copy(j):
        cols = pl.ds(j * cw, cw)
        return remote(
            snd.at[:, cols], car.at[:, cols], c_send.at[j], c_recv.at[j],
            {"sp": jnp.minimum(z + 1, n_sp - 1)},
        )

    def chain(j):
        cols = pl.ds(j * cw, cw)

        @pl.when(z == 0)
        def _():
            car[:, cols] = jnp.zeros((N, cw), BF16)

        @pl.when(z > 0)
        def _():
            chain_copy(j).wait_recv()

        @pl.when(z < n_sp - 1)
        def _():
            for p in range(j * cw // (2 * P_SIZE), (j + 1) * cw // (2 * P_SIZE)):
                pc = pair_cols(p)
                total = spread(whole, p, first_row) * car[:, pc].astype(F32) + st[:, pc]
                snd[:, pc] = total.astype(BF16)
            chain_copy(j).start()

    def inner(g):
        cb = dot(cm[:, g * N : (g + 1) * N], bm[:, g * N : (g + 1) * N], ((1,), (1,)))
        for p in range(g * per_group // 2, (g + 1) * per_group // 2):
            parts = []
            for h in (2 * p, 2 * p + 1):
                gap = jnp.where(lower, cum[:, h : h + 1] - cum_t[h : h + 1, :], -jnp.inf)
                parts.append(dot((cb * jnp.exp(gap)).astype(BF16), scaled[p]))
            y[:, pair_cols(p)] += jnp.where(first_head, parts[0], parts[1])

    for k in range(1, chunks):
        pump(1, k)
    for g in range(G):
        inner(g)
    for k in range(max(chunks, c_chunks)):
        if k < c_chunks:
            chain(k)
        if k < chunks:
            pump(2, k)
    finish(1)

    for g in range(G):
        cols = pl.ds(g * gw, gw)
        reached = dot(cm[:, g * N : (g + 1) * N], car[:, cols])
        gate = silu(dot(xe[pl.ds(HALO, tok), :], wz[:, cols]).astype(BF16).astype(F32))
        square = jnp.zeros((tok, 1), F32)
        first = g * per_group // 2
        for p in range(first, first + per_group // 2):
            here = slice((p - first) * 2 * P_SIZE, (p - first + 1) * 2 * P_SIZE)
            mixed = y[:, pair_cols(p)] + spread(reach, p, first_head) * reached[:, here]
            gated = mixed.astype(BF16).astype(F32) * gate[:, here]
            square = square + jnp.sum(gated * gated, axis=1, keepdims=True)
            y[:, pair_cols(p)] = gated
        inv = lax.rsqrt(square * (1.0 / gw) + EPSILON)
        nrm[:, cols] = (y[:, cols] * inv * scale_ref[:, cols]).astype(BF16)

    finish(2)
    fw = wf.shape[2]
    for d in range(n_dp):
        out_ref[:, d * fw : (d + 1) * fw] = dot(nrm[...], wf[d]).astype(BF16)

    for copy in sends:
        copy.wait_send()

    @pl.when(z < n_sp - 1)
    def _():
        halo_copy().wait_send()
        for j in range(c_chunks):
            chain_copy(j).wait_send()


def shards(
    dims,
    mixer_source_array,
    source_projection,
    gating_projection,
    entry_mapping_projection,
    readout_mapping_projection,
    increment_projection,
    source_conv_taps,
    entry_mapping_taps,
    readout_mapping_taps,
    increment_offsets,
    channel_damping_rate,
    bypass_coefficients,
    stride_multiplier,
    added_log_damping,
    norm_scale_factor,
    final_projection,
):
    n_grp, n_sp, n_dp, chunks, c_chunks = dims
    n_x = n_dp // 2
    hidden = mixer_source_array[0]
    tok, model = hidden.shape
    width = source_projection.shape[1]
    gn = G * N
    out_width = final_projection.shape[1] * n_dp
    dma = pltpu.SemaphoreType.DMA
    remote_srcs = max(n_x - 1, 1)
    vmem = pl.BlockSpec(memory_space=pltpu.VMEM)
    hbm = pl.BlockSpec(memory_space=pl.ANY)
    output = pl.pallas_call(
        functools.partial(kernel, dims),
        out_shape=jax.ShapeDtypeStruct((tok, out_width), BF16),
        in_specs=[hbm] * 4 + [vmem] * 12,
        out_specs=vmem,
        scratch_shapes=[
            pltpu.VMEM((HALO + tok, model), BF16),
            pltpu.VMEM((model, width), BF16),
            pltpu.VMEM((model, width), BF16),
            pltpu.VMEM((n_dp,) + final_projection.shape, BF16),
            pltpu.VMEM((HALO + tok, 2 * gn), F32),
            pltpu.VMEM((HALO + tok, width), F32),
            pltpu.VMEM((tok, gn), BF16),
            pltpu.VMEM((tok, gn), BF16),
            pltpu.VMEM((tok, width), BF16),
            pltpu.VMEM((tok, width), BF16),
            pltpu.VMEM((tok, width), F32),
            pltpu.VMEM((N, width), F32),
            pltpu.VMEM((N, width), BF16),
            pltpu.VMEM((N, width), BF16),
            pltpu.VMEM((tok, width), BF16),
            dma((4,)),
            dma,
            dma,
            dma((3, remote_srcs, chunks)),
            dma((3, remote_srcs, chunks)),
            dma((3, remote_srcs, chunks)),
            dma((3, remote_srcs)),
            dma((3, 2 * n_x - 1)),
            dma((3,)),
            dma((c_chunks,)),
            dma((c_chunks,)),
        ],
        compiler_params=pltpu.CompilerParams(
            collective_id=0, has_side_effects=True, vmem_limit_bytes=56 * 1024 * 1024
        ),
    )(
        hidden,
        source_projection,
        gating_projection,
        final_projection,
        entry_mapping_projection,
        readout_mapping_projection,
        increment_projection,
        source_conv_taps,
        entry_mapping_taps,
        readout_mapping_taps,
        increment_offsets[None],
        channel_damping_rate[None],
        bypass_coefficients[None],
        stride_multiplier,
        added_log_damping,
        norm_scale_factor[None],
    )
    return output[None]


def solution(mesh):
    n_grp, n_sp, n_dp = (mesh.shape[a] for a in ("grp", "sp", "dp"))
    chunks = 4 if n_dp <= 4 else 1
    return jax.shard_map(
        functools.partial(shards, (n_grp, n_sp, n_dp, chunks, 4)),
        mesh=mesh,
        in_specs=(
            P(("grp", "dp"), "sp", None),
            P("dp", None),
            P("dp", None),
            P(),
            P(),
            P(),
            P(),
            P(),
            P(),
            P(),
            P(),
            P(),
            P(("grp", "dp"), None),
            P(("grp", "dp"), None, None),
            P(),
            P(None, "dp"),
        ),
        out_specs=P(("grp", "dp"), "sp", None),
        check_vma=False,
    )
```

```python
import functools

import jax
import jax.numpy as jnp
from jax import lax
from jax.experimental import pallas as pl
from jax.experimental.pallas import tpu as pltpu
from jax.sharding import PartitionSpec as P

P_SIZE = 64
N = 128
G = 2
CONV_W = 4
EPSILON = 1e-06
HIGH = lax.Precision.HIGHEST
MESH = pl.DeviceIdType.MESH
HALO = 16
F32 = jnp.float32
BF16 = jnp.bfloat16


def dot(a, b, dims=((1,), (0,)), precision=None):
    return lax.dot_general(a, b, (dims, ((), ())), precision=precision, preferred_element_type=F32)


def silu(v):
    return v * (1.0 / (1.0 + jnp.exp(-v)))


def kernel(
    dims,
    x_hbm,
    wx_hbm,
    wz_hbm,
    wf_hbm,
    wb_hbm,
    wc_hbm,
    wdt_hbm,
    tx_ref,
    tb_ref,
    tc_ref,
    off_ref,
    rate_ref,
    skip_ref,
    stride_ref,
    damp_ref,
    scale_ref,
    out_hbm,
    xe,
    wx,
    wz,
    wf,
    pbc,
    px,
    bm,
    cm,
    xs,
    sc,
    y,
    st,
    car,
    snd,
    nrm,
    out_ref,
    wbc,
    wdt,
    loc_sem,
    halo_send,
    halo_recv,
    x_send,
    x_recv,
    y_send,
    y_recv,
    z_send,
    z_recv,
    d_send,
    d_recv,
    c_send,
    c_recv,
    o_sem,
):
    n_grp, n_sp, n_dp, c_chunks = dims
    n_x = n_dp // 2
    grp, z, dp = (lax.axis_index(a) for a in ("grp", "sp", "dp"))
    xi, core = dp // 2, dp % 2
    tok = out_ref.shape[0]
    width = xs.shape[1]
    heads = off_ref.shape[1]
    per_group = heads // G
    gw = width // G
    partner = {"dp": xi * 2 + 1 - core}
    y_peer = {"grp": 1 - grp}
    zb = z % 2
    z_peer = {"sp": z + 1 - 2 * zb}
    srcs = (wx_hbm, wz_hbm, wf_hbm)

    def at(w, owner, start, rows):
        if w == 2:
            return wf.at[owner, pl.ds(start, rows)]
        ref = (wx, wz)[w]
        return ref.at[pl.ds(pl.multiple_of(owner * srcs[w].shape[0] + start, 16), rows)]

    barrier = pltpu.get_barrier_semaphore()
    peers = [partner, y_peer]
    peers += [{"dp": lax.rem(xi + o, n_x) * 2 + core} for o in range(1, n_x)]
    for peer in peers:
        pl.semaphore_signal(barrier, inc=1, device_id=peer, device_id_type=MESH)

    @pl.when(z > 0)
    def _():
        pl.semaphore_signal(barrier, inc=1, device_id={"sp": z - 1}, device_id_type=MESH)

    @pl.when(z < n_sp - 1)
    def _():
        pl.semaphore_signal(barrier, inc=1, device_id={"sp": z + 1}, device_id_type=MESH)

    gn = G * N
    x_copy = pltpu.make_async_copy(x_hbm, xe.at[pl.ds(HALO, tok)], loc_sem.at[3])
    x_copy.start()
    maps = [
        pltpu.make_async_copy(wb_hbm, wbc.at[:, pl.ds(0, gn)], loc_sem.at[4]),
        pltpu.make_async_copy(wc_hbm, wbc.at[:, pl.ds(gn, gn)], loc_sem.at[5]),
        pltpu.make_async_copy(wdt_hbm, wdt, loc_sem.at[6]),
    ]
    for copy in maps:
        copy.start()
    own = []
    for w in range(3):
        copy = pltpu.make_async_copy(srcs[w], at(w, dp, 0, srcs[w].shape[0]), loc_sem.at[w])
        copy.start()
        own.append(copy)

    pl.semaphore_wait(barrier, len(peers) + jnp.minimum(z, 1) + jnp.minimum(n_sp - 1 - z, 1))

    def remote(src, dst, send, recv, peer):
        return pltpu.make_async_remote_copy(
            src_ref=src, dst_ref=dst, send_sem=send, recv_sem=recv,
            device_id=peer, device_id_type=MESH,
        )

    def halo_copy():
        return remote(
            x_hbm.at[pl.ds(tok - HALO, HALO)], xe.at[pl.ds(0, HALO)],
            halo_send, halo_recv, {"sp": jnp.minimum(z + 1, n_sp - 1)},
        )

    @pl.when(z < n_sp - 1)
    def _():
        halo_copy().start()

    sends = []

    def half_of(w):
        return srcs[w].shape[0] // 8

    def owner_of(o):
        return lax.rem(xi - o + n_x, n_x) * 2 + core

    own_q = grp * 2 + zb
    y_q = (1 - grp) * 2 + zb
    z_q = grp * 2 + 1 - zb
    far_q = (1 - grp) * 2 + 1 - zb

    def x_piece(w, o, k, owner, src=None):
        rows = half_of(w)
        start = far_q * 2 * rows + rows if k == 2 else own_q * 2 * rows + k * rows
        place = at(w, owner, start, rows)
        if src is not None:
            src = src.at[pl.ds(pl.multiple_of(start, 16), rows)]
        return remote(
            place if src is None else src, place,
            x_send.at[w, o - 1, k], x_recv.at[w, o - 1, k],
            {"dp": lax.rem(xi + o, n_x) * 2 + core},
        )

    def y_piece(w, o, k, quarter, part):
        place = at(w, owner_of(o), (quarter * 2 + part) * half_of(w), half_of(w))
        return remote(place, place, y_send.at[w, o - 1, k], y_recv.at[w, o - 1, k], y_peer)

    def z_piece(w, o, k, quarter):
        place = at(w, owner_of(o), (quarter * 2 + k) * half_of(w), half_of(w))
        return remote(place, place, z_send.at[w, o - 1, k], z_recv.at[w, o - 1, k], z_peer)

    def d_piece(w, o, k, quarter):
        place = at(w, owner_of(o), quarter * 2 * half_of(w), 2 * half_of(w))
        return remote(place, place, d_send.at[w, o, k], d_recv.at[w], partner)

    def start(copy):
        copy.start()
        sends.append(copy)

    for w in range(3):
        for k in range(3):
            for o in range(1, n_x):
                start(x_piece(w, o, k, dp, srcs[w]))
        rows = srcs[w].shape[0]
        start(remote(srcs[w], at(w, dp, 0, rows), d_send.at[w, 0, 0], d_recv.at[w], partner))

    def pump(w, k):
        for o in range(1, n_x):
            if k < 2:
                x_piece(w, o, k, owner_of(o)).wait_recv()
                start(y_piece(w, o, k, own_q, k))
                start(z_piece(w, o, k, own_q))
                if k == 1:
                    start(d_piece(w, o, 0, own_q))
            elif k == 2:
                z_piece(w, o, 0, z_q).wait_recv()
                start(y_piece(w, o, 2, z_q, 0))
            elif k == 3:
                z_piece(w, o, 1, z_q).wait_recv()
                start(d_piece(w, o, 1, z_q))
                y_piece(w, o, 0, y_q, 0).wait_recv()
                y_piece(w, o, 1, y_q, 1).wait_recv()
                start(d_piece(w, o, 2, y_q))
            else:
                y_piece(w, o, 2, far_q, 0).wait_recv()
                x_piece(w, o, 2, owner_of(o)).wait_recv()
                start(d_piece(w, o, 3, far_q))

    def finish(w):
        own[w].wait()
        if w == 2:
            place = wf.at[pl.ds(0, n_x)]
        else:
            place = (wx, wz)[w].at[pl.ds(0, n_x * srcs[w].shape[0])]
        remote(place, place, d_send.at[w, 0, 0], d_recv.at[w], partner).wait_recv()

    @pl.when(z == 0)
    def _():
        xe[pl.ds(0, HALO), :] = jnp.zeros((HALO, xe.shape[1]), BF16)

    @pl.when(z > 0)
    def _():
        halo_copy().wait_recv()

    x_copy.wait()
    for copy in maps:
        copy.wait()
    pbc[...] = dot(xe[...], wbc[...]).astype(BF16).astype(F32)
    raw = dot(wdt[...], xe[pl.ds(HALO, tok), :], ((1,), (1,))).astype(BF16).astype(F32)

    def conv(buf, cols, taps):
        total = taps[0:1, :] * buf[pl.ds(HALO - CONV_W + 1, tok), cols]
        for k in range(1, CONV_W):
            total = total + taps[k : k + 1, :] * buf[pl.ds(HALO - CONV_W + 1 + k, tok), cols]
        return silu(total).astype(BF16)

    bm[...] = conv(pbc, pl.ds(0, gn), tb_ref[...])
    cm[...] = conv(pbc, pl.ds(gn, gn), tc_ref[...])

    def square_iota(size):
        return [lax.broadcasted_iota(jnp.int32, (size, size), d) for d in (0, 1)]

    def column(ref):
        i, j = square_iota(heads)
        return jnp.sum(jnp.where(i == j, ref[...], 0.0), axis=1, keepdims=True)

    def my_positions(values):
        mine = values[:, 0:tok]
        for i in range(1, n_sp):
            mine = jnp.where(z == i, values[:, i * tok : (i + 1) * tok], mine)
        return mine

    pre = raw + column(off_ref)
    step_t = jnp.maximum(pre, 0.0) + jnp.log1p(jnp.exp(-jnp.abs(pre)))
    tempo = my_positions(stride_ref[...])
    keep = -column(rate_ref) * step_t * tempo + my_positions(damp_ref[0])
    row, col = square_iota(tok)
    lower = row >= col
    step = dot((row == col).astype(F32), step_t, ((1,), (1,)), HIGH)
    cum = dot(lower.astype(F32), keep, ((1,), (1,)), HIGH)
    cum_t = dot(keep, (row <= col).astype(F32), precision=HIGH)
    last = cum[tok - 1 : tok, :]
    to_end = jnp.exp(last - cum)
    reach = jnp.exp(cum)
    whole = jnp.exp(last)
    first_head = lax.broadcasted_iota(jnp.int32, (tok, 2 * P_SIZE), 1) < P_SIZE
    first_row = first_head[0:1, :]

    def spread(values, p, mask):
        return jnp.where(mask, values[:, 2 * p : 2 * p + 1], values[:, 2 * p + 1 : 2 * p + 2])

    def pair_cols(p):
        return pl.ds(p * 2 * P_SIZE, 2 * P_SIZE)

    for k in range(4):
        pump(0, k)
    pump(1, 0)
    pump(0, 4)
    finish(0)
    pump(1, 1)

    tile = 256

    def project_x(j, carry):
        cols = pl.ds(pl.multiple_of(j * tile, tile), tile)
        px[:, cols] = dot(xe[...], wx[:, cols]).astype(BF16).astype(F32)
        xs[:, cols] = conv(px, cols, tx_ref[:, cols])
        return carry

    lax.fori_loop(0, width // tile, project_x, 0)
    pump(1, 2)
    pump(1, 3)

    scaled = []
    for p in range(heads // 2):
        xp = xs[:, pair_cols(p)].astype(F32)
        s = (xp * spread(step, p, first_head)).astype(BF16)
        sc[:, pair_cols(p)] = (s.astype(F32) * spread(to_end, p, first_head)).astype(BF16)
        y[:, pair_cols(p)] = spread(skip_ref[...], p, first_row) * xp
        scaled.append(s)
    for g in range(G):
        cols = pl.ds(g * gw, gw)
        st[:, cols] = dot(bm[:, g * N : (g + 1) * N], sc[:, cols], ((0,), (0,)))

    cw = width // c_chunks

    def chain_copy(j):
        cols = pl.ds(j * cw, cw)
        return remote(
            snd.at[:, cols], car.at[:, cols], c_send.at[j], c_recv.at[j],
            {"sp": jnp.minimum(z + 1, n_sp - 1)},
        )

    def chain_first(j):
        cols = pl.ds(j * cw, cw)

        @pl.when(z == 0)
        def _():
            car[:, cols] = jnp.zeros((N, cw), BF16)
            snd[:, cols] = st[:, cols].astype(BF16)
            chain_copy(j).start()

    def chain(j):
        @pl.when(z > 0)
        def _():
            chain_copy(j).wait_recv()

            @pl.when(z < n_sp - 1)
            def _():
                for p in range(j * cw // (2 * P_SIZE), (j + 1) * cw // (2 * P_SIZE)):
                    pc = pair_cols(p)
                    total = spread(whole, p, first_row) * car[:, pc].astype(F32) + st[:, pc]
                    snd[:, pc] = total.astype(BF16)
                chain_copy(j).start()

    def inner(g):
        cb = dot(cm[:, g * N : (g + 1) * N], bm[:, g * N : (g + 1) * N], ((1,), (1,)))
        for p in range(g * per_group // 2, (g + 1) * per_group // 2):
            parts = []
            for h in (2 * p, 2 * p + 1):
                gap = jnp.where(lower, cum[:, h : h + 1] - cum_t[h : h + 1, :], -jnp.inf)
                parts.append(dot((cb * jnp.exp(gap)).astype(BF16), scaled[p]))
            y[:, pair_cols(p)] += jnp.where(first_head, parts[0], parts[1])

    for j in range(c_chunks):
        chain_first(j)
    inner(0)
    pump(2, 0)
    pump(1, 4)
    for g in range(1, G):
        inner(g)
    finish(1)
    chain(0)
    pump(2, 1)

    def project_z(j, carry):
        cols = pl.ds(pl.multiple_of(j * tile, tile), tile)
        acc = dot(xe[pl.ds(HALO, tok), :], wz[:, cols])
        px[pl.ds(0, tok), cols] = silu(acc.astype(BF16).astype(F32))
        return carry

    lax.fori_loop(0, width // tile, project_z, 0)
    for j in range(1, c_chunks - 1):
        chain(j)
    pump(2, 2)
    for j in range(max(1, c_chunks - 1), c_chunks):
        chain(j)

    for g in range(G):
        cols = pl.ds(g * gw, gw)
        reached = dot(cm[:, g * N : (g + 1) * N], car[:, cols])
        gate = px[pl.ds(0, tok), cols]
        square = jnp.zeros((tok, 1), F32)
        first = g * per_group // 2
        for p in range(first, first + per_group // 2):
            here = slice((p - first) * 2 * P_SIZE, (p - first + 1) * 2 * P_SIZE)
            mixed = y[:, pair_cols(p)] + spread(reach, p, first_head) * reached[:, here]
            gated = mixed.astype(BF16).astype(F32) * gate[:, here]
            square = square + jnp.sum(gated * gated, axis=1, keepdims=True)
            y[:, pair_cols(p)] = gated
        inv = lax.rsqrt(square * (1.0 / gw) + EPSILON)
        nrm[:, cols] = (y[:, cols] * inv * scale_ref[:, cols]).astype(BF16)

    pump(2, 3)
    pump(2, 4)
    finish(2)
    fw = wf.shape[2]
    for d in range(n_dp):
        out_ref[:, d * fw : (d + 1) * fw] = dot(nrm[...], wf[d]).astype(BF16)
        part = pl.ds(d * fw, fw)
        pltpu.make_async_copy(out_ref.at[:, part], out_hbm.at[:, part], o_sem.at[d]).start()
    for d in range(n_dp):
        part = pl.ds(d * fw, fw)
        pltpu.make_async_copy(out_ref.at[:, part], out_hbm.at[:, part], o_sem.at[d]).wait()

    for copy in sends:
        copy.wait_send()

    @pl.when(z < n_sp - 1)
    def _():
        halo_copy().wait_send()
        for j in range(c_chunks):
            chain_copy(j).wait_send()


def shards(
    dims,
    mixer_source_array,
    source_projection,
    gating_projection,
    entry_mapping_projection,
    readout_mapping_projection,
    increment_projection,
    source_conv_taps,
    entry_mapping_taps,
    readout_mapping_taps,
    increment_offsets,
    channel_damping_rate,
    bypass_coefficients,
    stride_multiplier,
    added_log_damping,
    norm_scale_factor,
    final_projection,
):
    n_grp, n_sp, n_dp, c_chunks = dims
    n_x = n_dp // 2
    hidden = mixer_source_array[0]
    tok, model = hidden.shape
    width = source_projection.shape[1]
    gn = G * N
    out_width = final_projection.shape[1] * n_dp
    dma = pltpu.SemaphoreType.DMA
    remote_srcs = max(n_x - 1, 1)
    vmem = pl.BlockSpec(memory_space=pltpu.VMEM)
    hbm = pl.BlockSpec(memory_space=pl.ANY)
    output = pl.pallas_call(
        functools.partial(kernel, dims),
        out_shape=jax.ShapeDtypeStruct((tok, out_width), BF16),
        in_specs=[hbm] * 7 + [vmem] * 9,
        out_specs=hbm,
        scratch_shapes=[
            pltpu.VMEM((HALO + tok, model), BF16),
            pltpu.VMEM((model, width), BF16),
            pltpu.VMEM((model, width), BF16),
            pltpu.VMEM((n_dp,) + final_projection.shape, BF16),
            pltpu.VMEM((HALO + tok, 2 * gn), F32),
            pltpu.VMEM((HALO + tok, width), F32),
            pltpu.VMEM((tok, gn), BF16),
            pltpu.VMEM((tok, gn), BF16),
            pltpu.VMEM((tok, width), BF16),
            pltpu.VMEM((tok, width), BF16),
            pltpu.VMEM((tok, width), F32),
            pltpu.VMEM((N, width), F32),
            pltpu.VMEM((N, width), BF16),
            pltpu.VMEM((N, width), BF16),
            pltpu.VMEM((tok, width), BF16),
            pltpu.VMEM((tok, out_width), BF16),
            pltpu.VMEM((model, 2 * gn), BF16),
            pltpu.VMEM((increment_projection.shape[1], model), BF16),
            dma((7,)),
            dma,
            dma,
            dma((3, remote_srcs, 3)),
            dma((3, remote_srcs, 3)),
            dma((3, remote_srcs, 3)),
            dma((3, remote_srcs, 3)),
            dma((3, remote_srcs, 2)),
            dma((3, remote_srcs, 2)),
            dma((3, n_x, 4)),
            dma((3,)),
            dma((c_chunks,)),
            dma((c_chunks,)),
            dma((n_dp,)),
        ],
        compiler_params=pltpu.CompilerParams(
            collective_id=0, has_side_effects=True, vmem_limit_bytes=56 * 1024 * 1024
        ),
    )(
        hidden,
        source_projection,
        gating_projection,
        final_projection,
        entry_mapping_projection,
        readout_mapping_projection,
        increment_projection.T,
        source_conv_taps,
        entry_mapping_taps,
        readout_mapping_taps,
        increment_offsets[None],
        channel_damping_rate[None],
        bypass_coefficients[None],
        stride_multiplier,
        jnp.swapaxes(added_log_damping, 1, 2),
        norm_scale_factor[None],
    )
    return output[None]


def solution(mesh):
    n_grp, n_sp, n_dp = (mesh.shape[a] for a in ("grp", "sp", "dp"))
    return jax.shard_map(
        functools.partial(shards, (n_grp, n_sp, n_dp, 4)),
        mesh=mesh,
        in_specs=(
            P(("grp", "dp"), "sp", None),
            P("dp", None),
            P("dp", None),
            P(),
            P(),
            P(),
            P(),
            P(),
            P(),
            P(),
            P(),
            P(),
            P(("grp", "dp"), None),
            P(("grp", "dp"), None, None),
            P(),
            P(None, "dp"),
        ),
        out_specs=P(("grp", "dp"), "sp", None),
        check_vma=False,
    )
```

```python
import functools

import jax
import jax.numpy as jnp
from jax import lax
from jax.experimental import pallas as pl
from jax.experimental.pallas import tpu as pltpu
from jax.sharding import PartitionSpec as P

P_SIZE = 64
N = 128
G = 2
CONV_W = 4
EPSILON = 1e-06
HIGH = lax.Precision.HIGHEST
MESH = pl.DeviceIdType.MESH
HALO = 16
F32 = jnp.float32
BF16 = jnp.bfloat16


def dot(a, b, dims=((1,), (0,)), precision=None):
    return lax.dot_general(a, b, (dims, ((), ())), precision=precision, preferred_element_type=F32)


def silu(v):
    return v * (1.0 / (1.0 + jnp.exp(-v)))


def kernel(
    dims,
    x_hbm,
    wx_hbm,
    wz_hbm,
    wf_hbm,
    wb_hbm,
    wc_hbm,
    wdt_hbm,
    tx_ref,
    tb_ref,
    tc_ref,
    off_ref,
    rate_ref,
    skip_ref,
    stride_ref,
    damp_ref,
    scale_ref,
    out_hbm,
    xe,
    wx,
    wz,
    wf,
    pbc,
    px,
    bm,
    cm,
    xs,
    sc,
    y,
    st,
    car,
    snd,
    nrm,
    out_ref,
    wbc,
    wdt,
    loc_sem,
    halo_send,
    halo_recv,
    x_send,
    x_recv,
    y_send,
    y_recv,
    z_send,
    z_recv,
    d_send,
    d_recv,
    c_send,
    c_recv,
    o_sem,
):
    n_grp, n_sp, n_dp, c_chunks = dims
    n_x = n_dp // 2
    grp, z, dp = (lax.axis_index(a) for a in ("grp", "sp", "dp"))
    xi, core = dp // 2, dp % 2
    tok = out_ref.shape[0]
    width = xs.shape[1]
    heads = off_ref.shape[1]
    per_group = heads // G
    gw = width // G
    partner = {"dp": xi * 2 + 1 - core}
    y_peer = {"grp": 1 - grp}
    zb = z % 2
    z_peer = {"sp": z + 1 - 2 * zb}
    srcs = (wx_hbm, wz_hbm, wf_hbm)

    def at(w, owner, start, rows):
        if w == 2:
            return wf.at[owner, pl.ds(start, rows)]
        ref = (wx, wz)[w]
        return ref.at[pl.ds(pl.multiple_of(owner * srcs[w].shape[0] + start, 16), rows)]

    barrier = pltpu.get_barrier_semaphore()
    peers = [partner, y_peer]
    peers += [{"dp": lax.rem(xi + o, n_x) * 2 + core} for o in range(1, n_x)]
    for peer in peers:
        pl.semaphore_signal(barrier, inc=1, device_id=peer, device_id_type=MESH)

    @pl.when(z > 0)
    def _():
        pl.semaphore_signal(barrier, inc=1, device_id={"sp": z - 1}, device_id_type=MESH)

    @pl.when(z < n_sp - 1)
    def _():
        pl.semaphore_signal(barrier, inc=1, device_id={"sp": z + 1}, device_id_type=MESH)

    gn = G * N
    x_copy = pltpu.make_async_copy(x_hbm, xe.at[pl.ds(HALO, tok)], loc_sem.at[3])
    x_copy.start()
    maps = [
        pltpu.make_async_copy(wb_hbm, wbc.at[:, pl.ds(0, gn)], loc_sem.at[4]),
        pltpu.make_async_copy(wc_hbm, wbc.at[:, pl.ds(gn, gn)], loc_sem.at[5]),
        pltpu.make_async_copy(wdt_hbm, wdt, loc_sem.at[6]),
    ]
    for copy in maps:
        copy.start()
    own = []
    for w in range(3):
        copy = pltpu.make_async_copy(srcs[w], at(w, dp, 0, srcs[w].shape[0]), loc_sem.at[w])
        copy.start()
        own.append(copy)

    pl.semaphore_wait(barrier, len(peers) + jnp.minimum(z, 1) + jnp.minimum(n_sp - 1 - z, 1))

    def remote(src, dst, send, recv, peer):
        return pltpu.make_async_remote_copy(
            src_ref=src, dst_ref=dst, send_sem=send, recv_sem=recv,
            device_id=peer, device_id_type=MESH,
        )

    def halo_copy():
        return remote(
            x_hbm.at[pl.ds(tok - HALO, HALO)], xe.at[pl.ds(0, HALO)],
            halo_send, halo_recv, {"sp": jnp.minimum(z + 1, n_sp - 1)},
        )

    @pl.when(z < n_sp - 1)
    def _():
        halo_copy().start()

    sends = []

    def half_of(w):
        return srcs[w].shape[0] // 8

    def owner_of(o):
        return lax.rem(xi - o + n_x, n_x) * 2 + core

    own_q = grp * 2 + zb
    y_q = (1 - grp) * 2 + zb
    z_q = grp * 2 + 1 - zb
    far_q = (1 - grp) * 2 + 1 - zb

    def x_piece(w, o, k, owner, src=None):
        rows = half_of(w)
        start = far_q * 2 * rows + rows if k == 2 else own_q * 2 * rows + k * rows
        place = at(w, owner, start, rows)
        if src is not None:
            src = src.at[pl.ds(pl.multiple_of(start, 16), rows)]
        return remote(
            place if src is None else src, place,
            x_send.at[w, o - 1, k], x_recv.at[w, o - 1, k],
            {"dp": lax.rem(xi + o, n_x) * 2 + core},
        )

    def y_piece(w, o, k, quarter, part):
        place = at(w, owner_of(o), (quarter * 2 + part) * half_of(w), half_of(w))
        return remote(place, place, y_send.at[w, o - 1, k], y_recv.at[w, o - 1, k], y_peer)

    def z_piece(w, o, k, quarter):
        place = at(w, owner_of(o), (quarter * 2 + k) * half_of(w), half_of(w))
        return remote(place, place, z_send.at[w, o - 1, k], z_recv.at[w, o - 1, k], z_peer)

    def d_piece(w, o, k, quarter):
        place = at(w, owner_of(o), quarter * 2 * half_of(w), 2 * half_of(w))
        return remote(place, place, d_send.at[w, o, k], d_recv.at[w, 1], partner)

    def start(copy):
        copy.start()
        sends.append(copy)

    for w in range(3):
        for k in range(3):
            for o in range(1, n_x):
                start(x_piece(w, o, k, dp, srcs[w]))
        rows = srcs[w].shape[0]
        start(remote(srcs[w], at(w, dp, 0, rows), d_send.at[w, 0, 0], d_recv.at[w, 0], partner))

    def pump(w, k):
        for o in range(1, n_x):
            if k < 2:
                x_piece(w, o, k, owner_of(o)).wait_recv()
                start(y_piece(w, o, k, own_q, k))
                start(z_piece(w, o, k, own_q))
                if k == 1:
                    start(d_piece(w, o, 0, own_q))
            elif k == 2:
                z_piece(w, o, 0, z_q).wait_recv()
                start(y_piece(w, o, 2, z_q, 0))
            elif k == 3:
                z_piece(w, o, 1, z_q).wait_recv()
                start(d_piece(w, o, 1, z_q))
                y_piece(w, o, 0, y_q, 0).wait_recv()
                y_piece(w, o, 1, y_q, 1).wait_recv()
                start(d_piece(w, o, 2, y_q))
            else:
                y_piece(w, o, 2, far_q, 0).wait_recv()
                x_piece(w, o, 2, owner_of(o)).wait_recv()
                start(d_piece(w, o, 3, far_q))

    def finish_near(w):
        own[w].wait()
        place = at(w, dp, 0, srcs[w].shape[0])
        remote(place, place, d_send.at[w, 0, 0], d_recv.at[w, 0], partner).wait_recv()

    def finish_far(w):
        if w == 2:
            place = wf.at[pl.ds(0, n_x - 1)]
        else:
            place = (wx, wz)[w].at[pl.ds(0, (n_x - 1) * srcs[w].shape[0])]
        remote(place, place, d_send.at[w, 1, 0], d_recv.at[w, 1], partner).wait_recv()

    depth = 2 * wx_hbm.shape[0]

    def chip_rows(o):
        return pl.ds(pl.multiple_of(lax.rem(xi - o + n_x, n_x) * depth, 128), depth)

    @pl.when(z == 0)
    def _():
        xe[pl.ds(0, HALO), :] = jnp.zeros((HALO, xe.shape[1]), BF16)

    @pl.when(z > 0)
    def _():
        halo_copy().wait_recv()

    x_copy.wait()
    for copy in maps:
        copy.wait()
    pbc[...] = dot(xe[...], wbc[...]).astype(BF16).astype(F32)
    raw = dot(wdt[...], xe[pl.ds(HALO, tok), :], ((1,), (1,))).astype(BF16).astype(F32)

    def conv(buf, cols, taps):
        total = taps[0:1, :] * buf[pl.ds(HALO - CONV_W + 1, tok), cols]
        for k in range(1, CONV_W):
            total = total + taps[k : k + 1, :] * buf[pl.ds(HALO - CONV_W + 1 + k, tok), cols]
        return silu(total).astype(BF16)

    bm[...] = conv(pbc, pl.ds(0, gn), tb_ref[...])
    cm[...] = conv(pbc, pl.ds(gn, gn), tc_ref[...])

    def square_iota(size):
        return [lax.broadcasted_iota(jnp.int32, (size, size), d) for d in (0, 1)]

    def column(ref):
        i, j = square_iota(heads)
        return jnp.sum(jnp.where(i == j, ref[...], 0.0), axis=1, keepdims=True)

    def my_positions(values):
        mine = values[:, 0:tok]
        for i in range(1, n_sp):
            mine = jnp.where(z == i, values[:, i * tok : (i + 1) * tok], mine)
        return mine

    pre = raw + column(off_ref)
    step_t = jnp.maximum(pre, 0.0) + jnp.log1p(jnp.exp(-jnp.abs(pre)))
    tempo = my_positions(stride_ref[...])
    keep = -column(rate_ref) * step_t * tempo + my_positions(damp_ref[0])
    row, col = square_iota(tok)
    lower = row >= col
    step = dot((row == col).astype(F32), step_t, ((1,), (1,)), HIGH)
    cum = dot(lower.astype(F32), keep, ((1,), (1,)), HIGH)
    cum_t = dot(keep, (row <= col).astype(F32), precision=HIGH)
    last = cum[tok - 1 : tok, :]
    to_end = jnp.exp(last - cum)
    reach = jnp.exp(cum)
    whole = jnp.exp(last)
    first_head = lax.broadcasted_iota(jnp.int32, (tok, 2 * P_SIZE), 1) < P_SIZE
    first_row = first_head[0:1, :]

    def spread(values, p, mask):
        return jnp.where(mask, values[:, 2 * p : 2 * p + 1], values[:, 2 * p + 1 : 2 * p + 2])

    def pair_cols(p):
        return pl.ds(p * 2 * P_SIZE, 2 * P_SIZE)

    tile = 256

    def tiles(body):
        def run(j, carry):
            body(pl.ds(pl.multiple_of(j * tile, tile), tile))
            return carry

        lax.fori_loop(0, width // tile, run, 0)

    def near_x(cols):
        px[:, cols] = dot(xe[:, chip_rows(0)], wx[chip_rows(0), cols])

    def far_x(cols):
        acc = px[:, cols]
        for o in range(1, n_x):
            acc = acc + dot(xe[:, chip_rows(o)], wx[chip_rows(o), cols])
        px[:, cols] = acc.astype(BF16).astype(F32)
        xs[:, cols] = conv(px, cols, tx_ref[:, cols])

    rows = pl.ds(HALO, tok)

    def near_z(cols):
        px[pl.ds(0, tok), cols] = dot(xe[rows, chip_rows(0)], wz[chip_rows(0), cols])

    def far_z(cols):
        acc = px[pl.ds(0, tok), cols]
        for o in range(1, n_x):
            acc = acc + dot(xe[rows, chip_rows(o)], wz[chip_rows(o), cols])
        px[pl.ds(0, tok), cols] = silu(acc.astype(BF16).astype(F32))

    pump(0, 0)
    pump(0, 1)
    finish_near(0)
    tiles(near_x)
    pump(0, 2)
    pump(0, 3)
    pump(1, 0)
    pump(0, 4)
    finish_far(0)
    pump(1, 1)
    tiles(far_x)
    pump(1, 2)

    scaled = []
    for p in range(heads // 2):
        xp = xs[:, pair_cols(p)].astype(F32)
        s = (xp * spread(step, p, first_head)).astype(BF16)
        sc[:, pair_cols(p)] = (s.astype(F32) * spread(to_end, p, first_head)).astype(BF16)
        y[:, pair_cols(p)] = spread(skip_ref[...], p, first_row) * xp
        scaled.append(s)
    for g in range(G):
        cols = pl.ds(g * gw, gw)
        st[:, cols] = dot(bm[:, g * N : (g + 1) * N], sc[:, cols], ((0,), (0,)))

    cw = width // c_chunks

    def chain_copy(j):
        cols = pl.ds(j * cw, cw)
        return remote(
            snd.at[:, cols], car.at[:, cols], c_send.at[j], c_recv.at[j],
            {"sp": jnp.minimum(z + 1, n_sp - 1)},
        )

    def chain_first(j):
        cols = pl.ds(j * cw, cw)

        @pl.when(z == 0)
        def _():
            car[:, cols] = jnp.zeros((N, cw), BF16)
            snd[:, cols] = st[:, cols].astype(BF16)
            chain_copy(j).start()

    def chain(j):
        @pl.when(z > 0)
        def _():
            chain_copy(j).wait_recv()

            @pl.when(z < n_sp - 1)
            def _():
                for p in range(j * cw // (2 * P_SIZE), (j + 1) * cw // (2 * P_SIZE)):
                    pc = pair_cols(p)
                    total = spread(whole, p, first_row) * car[:, pc].astype(F32) + st[:, pc]
                    snd[:, pc] = total.astype(BF16)
                chain_copy(j).start()

    def inner(g):
        cb = dot(cm[:, g * N : (g + 1) * N], bm[:, g * N : (g + 1) * N], ((1,), (1,)))
        for p in range(g * per_group // 2, (g + 1) * per_group // 2):
            parts = []
            for h in (2 * p, 2 * p + 1):
                gap = jnp.where(lower, cum[:, h : h + 1] - cum_t[h : h + 1, :], -jnp.inf)
                parts.append(dot((cb * jnp.exp(gap)).astype(BF16), scaled[p]))
            y[:, pair_cols(p)] += jnp.where(first_head, parts[0], parts[1])

    def chain_slot(slot):
        @pl.when(jnp.minimum(z, 3) == slot)
        def _():
            for j in range(c_chunks):
                chain(j)

    for j in range(c_chunks):
        chain_first(j)
    pump(1, 3)
    pump(2, 0)
    inner(0)
    pump(1, 4)
    chain_slot(1)
    pump(2, 1)
    inner(1)
    pump(2, 2)
    chain_slot(2)
    finish_near(1)
    tiles(near_z)
    finish_far(1)
    tiles(far_z)
    chain_slot(3)

    for g in range(G):
        cols = pl.ds(g * gw, gw)
        reached = dot(cm[:, g * N : (g + 1) * N], car[:, cols])
        gate = px[pl.ds(0, tok), cols]
        square = jnp.zeros((tok, 1), F32)
        first = g * per_group // 2
        for p in range(first, first + per_group // 2):
            here = slice((p - first) * 2 * P_SIZE, (p - first + 1) * 2 * P_SIZE)
            mixed = y[:, pair_cols(p)] + spread(reach, p, first_head) * reached[:, here]
            gated = mixed.astype(BF16).astype(F32) * gate[:, here]
            square = square + jnp.sum(gated * gated, axis=1, keepdims=True)
            y[:, pair_cols(p)] = gated
        inv = lax.rsqrt(square * (1.0 / gw) + EPSILON)
        nrm[:, cols] = (y[:, cols] * inv * scale_ref[:, cols]).astype(BF16)

    fw = wf.shape[2]

    def finish_output(d):
        part = pl.ds(pl.multiple_of(d * fw, 128), fw)
        out_ref[:, part] = dot(nrm[...], wf[d]).astype(BF16)
        pltpu.make_async_copy(out_ref.at[:, part], out_hbm.at[:, part], o_sem.at[d]).start()

    pump(2, 3)
    finish_near(2)
    finish_output(dp)
    finish_output(dp + 1 - 2 * core)
    pump(2, 4)
    for o in range(1, n_x):
        finish_output(owner_of(o))
    finish_far(2)
    for o in range(1, n_x):
        finish_output(owner_of(o) + 1 - 2 * core)
    for d in range(n_dp):
        part = pl.ds(d * fw, fw)
        pltpu.make_async_copy(out_ref.at[:, part], out_hbm.at[:, part], o_sem.at[d]).wait()

    for copy in sends:
        copy.wait_send()

    @pl.when(z < n_sp - 1)
    def _():
        halo_copy().wait_send()
        for j in range(c_chunks):
            chain_copy(j).wait_send()


def shards(
    dims,
    mixer_source_array,
    source_projection,
    gating_projection,
    entry_mapping_projection,
    readout_mapping_projection,
    increment_projection,
    source_conv_taps,
    entry_mapping_taps,
    readout_mapping_taps,
    increment_offsets,
    channel_damping_rate,
    bypass_coefficients,
    stride_multiplier,
    added_log_damping,
    norm_scale_factor,
    final_projection,
):
    n_grp, n_sp, n_dp, c_chunks = dims
    n_x = n_dp // 2
    hidden = mixer_source_array[0]
    tok, model = hidden.shape
    width = source_projection.shape[1]
    gn = G * N
    out_width = final_projection.shape[1] * n_dp
    dma = pltpu.SemaphoreType.DMA
    remote_srcs = max(n_x - 1, 1)
    vmem = pl.BlockSpec(memory_space=pltpu.VMEM)
    hbm = pl.BlockSpec(memory_space=pl.ANY)
    output = pl.pallas_call(
        functools.partial(kernel, dims),
        out_shape=jax.ShapeDtypeStruct((tok, out_width), BF16),
        in_specs=[hbm] * 7 + [vmem] * 9,
        out_specs=hbm,
        scratch_shapes=[
            pltpu.VMEM((HALO + tok, model), BF16),
            pltpu.VMEM((model, width), BF16),
            pltpu.VMEM((model, width), BF16),
            pltpu.VMEM((n_dp,) + final_projection.shape, BF16),
            pltpu.VMEM((HALO + tok, 2 * gn), F32),
            pltpu.VMEM((HALO + tok, width), F32),
            pltpu.VMEM((tok, gn), BF16),
            pltpu.VMEM((tok, gn), BF16),
            pltpu.VMEM((tok, width), BF16),
            pltpu.VMEM((tok, width), BF16),
            pltpu.VMEM((tok, width), F32),
            pltpu.VMEM((N, width), F32),
            pltpu.VMEM((N, width), BF16),
            pltpu.VMEM((N, width), BF16),
            pltpu.VMEM((tok, width), BF16),
            pltpu.VMEM((tok, out_width), BF16),
            pltpu.VMEM((model, 2 * gn), BF16),
            pltpu.VMEM((increment_projection.shape[1], model), BF16),
            dma((7,)),
            dma,
            dma,
            dma((3, remote_srcs, 3)),
            dma((3, remote_srcs, 3)),
            dma((3, remote_srcs, 3)),
            dma((3, remote_srcs, 3)),
            dma((3, remote_srcs, 2)),
            dma((3, remote_srcs, 2)),
            dma((3, n_x, 4)),
            dma((3, 2)),
            dma((c_chunks,)),
            dma((c_chunks,)),
            dma((n_dp,)),
        ],
        compiler_params=pltpu.CompilerParams(
            collective_id=0, has_side_effects=True, vmem_limit_bytes=56 * 1024 * 1024
        ),
    )(
        hidden,
        source_projection,
        gating_projection,
        final_projection,
        entry_mapping_projection,
        readout_mapping_projection,
        increment_projection.T,
        source_conv_taps,
        entry_mapping_taps,
        readout_mapping_taps,
        increment_offsets[None],
        channel_damping_rate[None],
        bypass_coefficients[None],
        stride_multiplier,
        jnp.swapaxes(added_log_damping, 1, 2),
        norm_scale_factor[None],
    )
    return output[None]


def solution(mesh):
    n_grp, n_sp, n_dp = (mesh.shape[a] for a in ("grp", "sp", "dp"))
    return jax.shard_map(
        functools.partial(shards, (n_grp, n_sp, n_dp, 4)),
        mesh=mesh,
        in_specs=(
            P(("grp", "dp"), "sp", None),
            P("dp", None),
            P("dp", None),
            P(),
            P(),
            P(),
            P(),
            P(),
            P(),
            P(),
            P(),
            P(),
            P(("grp", "dp"), None),
            P(("grp", "dp"), None, None),
            P(),
            P(None, "dp"),
        ),
        out_specs=P(("grp", "dp"), "sp", None),
        check_vma=False,
    )
```

```python
import functools

import jax
import jax.numpy as jnp
from jax import lax
from jax.experimental import pallas as pl
from jax.experimental.pallas import tpu as pltpu
from jax.sharding import PartitionSpec as P

P_SIZE = 64
N = 128
G = 2
CONV_W = 4
EPSILON = 1e-06
HIGH = lax.Precision.HIGHEST
MESH = pl.DeviceIdType.MESH
HALO = 16
F32 = jnp.float32
BF16 = jnp.bfloat16


def dot(a, b, dims=((1,), (0,)), precision=None):
    return lax.dot_general(a, b, (dims, ((), ())), precision=precision, preferred_element_type=F32)


def silu(v):
    return v * (1.0 / (1.0 + jnp.exp(-v)))


def kernel(
    dims,
    x_hbm,
    wx_hbm,
    wz_hbm,
    wf_hbm,
    wb_hbm,
    wc_hbm,
    wdt_hbm,
    tx_ref,
    tb_ref,
    tc_ref,
    off_ref,
    rate_ref,
    skip_ref,
    stride_ref,
    damp_ref,
    scale_ref,
    out_hbm,
    xe,
    wx,
    wz,
    wf,
    pbc,
    px,
    bm,
    cm,
    xs,
    sc,
    y,
    st,
    car,
    snd,
    nrm,
    out_ref,
    wbc,
    wdt,
    loc_sem,
    halo_send,
    halo_recv,
    x_send,
    x_recv,
    y_send,
    y_recv,
    z_send,
    z_recv,
    d_send,
    d_recv,
    c_send,
    c_recv,
    o_sem,
):
    n_grp, n_sp, n_dp, c_chunks = dims
    n_x = n_dp // 2
    grp, z, dp = (lax.axis_index(a) for a in ("grp", "sp", "dp"))
    xi, core = dp // 2, dp % 2
    tok = out_ref.shape[0]
    width = xs.shape[1]
    heads = off_ref.shape[1]
    per_group = heads // G
    gw = width // G
    partner = {"dp": xi * 2 + 1 - core}
    y_peer = {"grp": 1 - grp}
    zb = z % 2
    z_peer = {"sp": z + 1 - 2 * zb}
    srcs = (wx_hbm, wz_hbm, wf_hbm)

    def at(w, owner, start, rows):
        if w == 2:
            return wf.at[owner, pl.ds(start, rows)]
        ref = (wx, wz)[w]
        return ref.at[pl.ds(pl.multiple_of(owner * srcs[w].shape[0] + start, 16), rows)]

    barrier = pltpu.get_barrier_semaphore()
    peers = [partner, y_peer]
    peers += [{"dp": lax.rem(xi + o, n_x) * 2 + core} for o in range(1, n_x)]
    for peer in peers:
        pl.semaphore_signal(barrier, inc=1, device_id=peer, device_id_type=MESH)

    @pl.when(z > 0)
    def _():
        pl.semaphore_signal(barrier, inc=1, device_id={"sp": z - 1}, device_id_type=MESH)

    @pl.when(z < n_sp - 1)
    def _():
        pl.semaphore_signal(barrier, inc=1, device_id={"sp": z + 1}, device_id_type=MESH)

    gn = G * N
    x_copy = pltpu.make_async_copy(x_hbm, xe.at[pl.ds(HALO, tok)], loc_sem.at[3])
    x_copy.start()
    maps = [
        pltpu.make_async_copy(wb_hbm, wbc.at[:, pl.ds(0, gn)], loc_sem.at[4]),
        pltpu.make_async_copy(wc_hbm, wbc.at[:, pl.ds(gn, gn)], loc_sem.at[5]),
        pltpu.make_async_copy(wdt_hbm, wdt, loc_sem.at[6]),
    ]
    for copy in maps:
        copy.start()
    own = []
    for w in range(3):
        copy = pltpu.make_async_copy(srcs[w], at(w, dp, 0, srcs[w].shape[0]), loc_sem.at[w])
        copy.start()
        own.append(copy)

    pl.semaphore_wait(barrier, len(peers) + jnp.minimum(z, 1) + jnp.minimum(n_sp - 1 - z, 1))

    def remote(src, dst, send, recv, peer):
        return pltpu.make_async_remote_copy(
            src_ref=src, dst_ref=dst, send_sem=send, recv_sem=recv,
            device_id=peer, device_id_type=MESH,
        )

    def halo_copy():
        return remote(
            x_hbm.at[pl.ds(tok - HALO, HALO)], xe.at[pl.ds(0, HALO)],
            halo_send, halo_recv, {"sp": jnp.minimum(z + 1, n_sp - 1)},
        )

    @pl.when(z < n_sp - 1)
    def _():
        halo_copy().start()

    sends = []

    def half_of(w):
        return srcs[w].shape[0] // 8

    def owner_of(o):
        return lax.rem(xi - o + n_x, n_x) * 2 + core

    own_q = grp * 2 + zb
    y_q = (1 - grp) * 2 + zb
    z_q = grp * 2 + 1 - zb
    far_q = (1 - grp) * 2 + 1 - zb

    def x_piece(w, o, k, owner, src=None):
        rows = half_of(w)
        start = far_q * 2 * rows + rows if k == 2 else own_q * 2 * rows + k * rows
        place = at(w, owner, start, rows)
        if src is not None:
            src = src.at[pl.ds(pl.multiple_of(start, 16), rows)]
        return remote(
            place if src is None else src, place,
            x_send.at[w, o - 1, k], x_recv.at[w, o - 1, k],
            {"dp": lax.rem(xi + o, n_x) * 2 + core},
        )

    def y_piece(w, o, k, quarter, part):
        place = at(w, owner_of(o), (quarter * 2 + part) * half_of(w), half_of(w))
        return remote(place, place, y_send.at[w, o - 1, k], y_recv.at[w, o - 1, k], y_peer)

    def z_piece(w, o, k, quarter):
        place = at(w, owner_of(o), (quarter * 2 + k) * half_of(w), half_of(w))
        return remote(place, place, z_send.at[w, o - 1, k], z_recv.at[w, o - 1, k], z_peer)

    def d_piece(w, o, k, quarter):
        place = at(w, owner_of(o), quarter * 2 * half_of(w), 2 * half_of(w))
        return remote(place, place, d_send.at[w, o, k], d_recv.at[w, 1], partner)

    def start(copy):
        copy.start()
        sends.append(copy)

    for w in range(3):
        for k in range(3):
            for o in range(1, n_x):
                start(x_piece(w, o, k, dp, srcs[w]))
        rows = srcs[w].shape[0]
        start(remote(srcs[w], at(w, dp, 0, rows), d_send.at[w, 0, 0], d_recv.at[w, 0], partner))

    def pump(w, k):
        for o in range(1, n_x):
            if k < 2:
                x_piece(w, o, k, owner_of(o)).wait_recv()
                start(y_piece(w, o, k, own_q, k))
                start(z_piece(w, o, k, own_q))
                if k == 1:
                    start(d_piece(w, o, 0, own_q))
            elif k == 2:
                z_piece(w, o, 0, z_q).wait_recv()
                start(y_piece(w, o, 2, z_q, 0))
            elif k == 3:
                z_piece(w, o, 1, z_q).wait_recv()
                start(d_piece(w, o, 1, z_q))
                y_piece(w, o, 0, y_q, 0).wait_recv()
                y_piece(w, o, 1, y_q, 1).wait_recv()
                start(d_piece(w, o, 2, y_q))
            else:
                y_piece(w, o, 2, far_q, 0).wait_recv()
                x_piece(w, o, 2, owner_of(o)).wait_recv()
                start(d_piece(w, o, 3, far_q))

    def finish_near(w):
        own[w].wait()
        place = at(w, dp, 0, srcs[w].shape[0])
        remote(place, place, d_send.at[w, 0, 0], d_recv.at[w, 0], partner).wait_recv()

    def finish_far(w):
        if w == 2:
            place = wf.at[pl.ds(0, n_x - 1)]
        else:
            place = (wx, wz)[w].at[pl.ds(0, (n_x - 1) * srcs[w].shape[0])]
        remote(place, place, d_send.at[w, 1, 0], d_recv.at[w, 1], partner).wait_recv()

    depth = 2 * wx_hbm.shape[0]

    def chip_rows(o):
        return pl.ds(pl.multiple_of(lax.rem(xi - o + n_x, n_x) * depth, 128), depth)

    @pl.when(z == 0)
    def _():
        xe[pl.ds(0, HALO), :] = jnp.zeros((HALO, xe.shape[1]), BF16)

    @pl.when(z > 0)
    def _():
        halo_copy().wait_recv()

    x_copy.wait()
    for copy in maps:
        copy.wait()
    pbc[...] = dot(xe[...], wbc[...]).astype(BF16).astype(F32)
    raw = dot(wdt[...], xe[pl.ds(HALO, tok), :], ((1,), (1,))).astype(BF16).astype(F32)

    def conv(buf, cols, taps):
        total = taps[0:1, :] * buf[pl.ds(HALO - CONV_W + 1, tok), cols]
        for k in range(1, CONV_W):
            total = total + taps[k : k + 1, :] * buf[pl.ds(HALO - CONV_W + 1 + k, tok), cols]
        return silu(total).astype(BF16)

    bm[...] = conv(pbc, pl.ds(0, gn), tb_ref[...])
    cm[...] = conv(pbc, pl.ds(gn, gn), tc_ref[...])

    def square_iota(size):
        return [lax.broadcasted_iota(jnp.int32, (size, size), d) for d in (0, 1)]

    def column(ref):
        i, j = square_iota(heads)
        return jnp.sum(jnp.where(i == j, ref[...], 0.0), axis=1, keepdims=True)

    def my_positions(values):
        mine = values[:, 0:tok]
        for i in range(1, n_sp):
            mine = jnp.where(z == i, values[:, i * tok : (i + 1) * tok], mine)
        return mine

    pre = raw + column(off_ref)
    step_t = jnp.maximum(pre, 0.0) + jnp.log1p(jnp.exp(-jnp.abs(pre)))
    tempo = my_positions(stride_ref[...])
    keep = -column(rate_ref) * step_t * tempo + my_positions(damp_ref[0])
    row, col = square_iota(tok)
    lower = row >= col
    step = dot((row == col).astype(F32), step_t, ((1,), (1,)), HIGH)
    cum = dot(lower.astype(F32), keep, ((1,), (1,)), HIGH)
    cum_t = dot(keep, (row <= col).astype(F32), precision=HIGH)
    last = cum[tok - 1 : tok, :]
    to_end = jnp.exp(last - cum)
    reach = jnp.exp(cum)
    whole = jnp.exp(last)
    first_head = lax.broadcasted_iota(jnp.int32, (tok, 2 * P_SIZE), 1) < P_SIZE
    first_row = first_head[0:1, :]

    def spread(values, p, mask):
        return jnp.where(mask, values[:, 2 * p : 2 * p + 1], values[:, 2 * p + 1 : 2 * p + 2])

    def pair_cols(p):
        return pl.ds(p * 2 * P_SIZE, 2 * P_SIZE)

    tile = 256

    def tiles(body):
        def run(j, carry):
            body(pl.ds(pl.multiple_of(j * tile, tile), tile))
            return carry

        lax.fori_loop(0, width // tile, run, 0)

    def near_x(cols):
        px[:, cols] = dot(xe[:, chip_rows(0)], wx[chip_rows(0), cols])

    def far_x(cols):
        acc = px[:, cols]
        for o in range(1, n_x):
            acc = acc + dot(xe[:, chip_rows(o)], wx[chip_rows(o), cols])
        px[:, cols] = acc.astype(BF16).astype(F32)
        xs[:, cols] = conv(px, cols, tx_ref[:, cols])

    rows = pl.ds(HALO, tok)

    def near_z(cols):
        px[pl.ds(0, tok), cols] = dot(xe[rows, chip_rows(0)], wz[chip_rows(0), cols])

    def far_z(cols):
        acc = px[pl.ds(0, tok), cols]
        for o in range(1, n_x):
            acc = acc + dot(xe[rows, chip_rows(o)], wz[chip_rows(o), cols])
        px[pl.ds(0, tok), cols] = silu(acc.astype(BF16).astype(F32))

    pump(0, 0)
    pump(0, 1)
    finish_near(0)
    tiles(near_x)
    pump(0, 2)
    pump(0, 3)
    pump(1, 0)
    pump(0, 4)
    finish_far(0)
    pump(1, 1)
    tiles(far_x)
    pump(1, 2)

    scaled = []
    cw = width // c_chunks

    def chain_copy(j):
        cols = pl.ds(j * cw, cw)
        return remote(
            snd.at[:, cols], car.at[:, cols], c_send.at[j], c_recv.at[j],
            {"sp": jnp.minimum(z + 1, n_sp - 1)},
        )

    def chain_first(j):
        cols = pl.ds(j * cw, cw)

        @pl.when(z == 0)
        def _():
            car[:, cols] = jnp.zeros((N, cw), BF16)
            snd[:, cols] = st[:, cols].astype(BF16)
            chain_copy(j).start()

    def chain(j):
        @pl.when(z > 0)
        def _():
            chain_copy(j).wait_recv()

            @pl.when(z < n_sp - 1)
            def _():
                for p in range(j * cw // (2 * P_SIZE), (j + 1) * cw // (2 * P_SIZE)):
                    pc = pair_cols(p)
                    total = spread(whole, p, first_row) * car[:, pc].astype(F32) + st[:, pc]
                    snd[:, pc] = total.astype(BF16)
                chain_copy(j).start()

    def inner(g):
        cb = dot(cm[:, g * N : (g + 1) * N], bm[:, g * N : (g + 1) * N], ((1,), (1,)))
        for p in range(g * per_group // 2, (g + 1) * per_group // 2):
            parts = []
            for h in (2 * p, 2 * p + 1):
                gap = jnp.where(lower, cum[:, h : h + 1] - cum_t[h : h + 1, :], -jnp.inf)
                parts.append(dot((cb * jnp.exp(gap)).astype(BF16), scaled[p]))
            bypass = spread(skip_ref[...], p, first_row) * xs[:, pair_cols(p)].astype(F32)
            y[:, pair_cols(p)] = jnp.where(first_head, parts[0], parts[1]) + bypass

    def local_state(g):
        for p in range(g * per_group // 2, (g + 1) * per_group // 2):
            xp = xs[:, pair_cols(p)].astype(F32)
            part = (xp * spread(step, p, first_head)).astype(BF16)
            sc[:, pair_cols(p)] = (part.astype(F32) * spread(to_end, p, first_head)).astype(BF16)
            scaled.append(part)
        cols = pl.ds(g * gw, gw)
        st[:, cols] = dot(bm[:, g * N : (g + 1) * N], sc[:, cols], ((0,), (0,)))
        for j in range(g * c_chunks // G, (g + 1) * c_chunks // G):
            chain_first(j)

    def chain_slot(slot):
        @pl.when(jnp.minimum(z, 3) == slot)
        def _():
            for j in range(c_chunks):
                chain(j)

    for g in range(G):
        local_state(g)
    pump(1, 3)
    pump(2, 0)
    inner(0)
    pump(1, 4)
    chain_slot(1)
    pump(2, 1)
    inner(1)
    pump(2, 2)
    chain_slot(2)
    finish_near(1)
    tiles(near_z)
    finish_far(1)
    tiles(far_z)
    chain_slot(3)

    for g in range(G):
        cols = pl.ds(g * gw, gw)
        reached = dot(cm[:, g * N : (g + 1) * N], car[:, cols])
        gate = px[pl.ds(0, tok), cols]
        square = jnp.zeros((tok, 1), F32)
        first = g * per_group // 2
        for p in range(first, first + per_group // 2):
            here = slice((p - first) * 2 * P_SIZE, (p - first + 1) * 2 * P_SIZE)
            mixed = y[:, pair_cols(p)] + spread(reach, p, first_head) * reached[:, here]
            gated = mixed.astype(BF16).astype(F32) * gate[:, here]
            square = square + jnp.sum(gated * gated, axis=1, keepdims=True)
            y[:, pair_cols(p)] = gated
        inv = lax.rsqrt(square * (1.0 / gw) + EPSILON)
        nrm[:, cols] = (y[:, cols] * inv * scale_ref[:, cols]).astype(BF16)

    fw = wf.shape[2]

    def finish_output(d):
        part = pl.ds(pl.multiple_of(d * fw, 128), fw)
        out_ref[:, part] = dot(nrm[...], wf[d]).astype(BF16)
        pltpu.make_async_copy(out_ref.at[:, part], out_hbm.at[:, part], o_sem.at[d]).start()

    pump(2, 3)
    finish_near(2)
    finish_output(dp)
    finish_output(dp + 1 - 2 * core)
    pump(2, 4)
    for o in range(1, n_x):
        finish_output(owner_of(o))
    finish_far(2)
    for o in range(1, n_x):
        finish_output(owner_of(o) + 1 - 2 * core)
    for d in range(n_dp):
        part = pl.ds(d * fw, fw)
        pltpu.make_async_copy(out_ref.at[:, part], out_hbm.at[:, part], o_sem.at[d]).wait()

    for copy in sends:
        copy.wait_send()

    @pl.when(z < n_sp - 1)
    def _():
        halo_copy().wait_send()
        for j in range(c_chunks):
            chain_copy(j).wait_send()


def shards(
    dims,
    mixer_source_array,
    source_projection,
    gating_projection,
    entry_mapping_projection,
    readout_mapping_projection,
    increment_projection,
    source_conv_taps,
    entry_mapping_taps,
    readout_mapping_taps,
    increment_offsets,
    channel_damping_rate,
    bypass_coefficients,
    stride_multiplier,
    added_log_damping,
    norm_scale_factor,
    final_projection,
):
    n_grp, n_sp, n_dp, c_chunks = dims
    n_x = n_dp // 2
    hidden = mixer_source_array[0]
    tok, model = hidden.shape
    width = source_projection.shape[1]
    gn = G * N
    out_width = final_projection.shape[1] * n_dp
    dma = pltpu.SemaphoreType.DMA
    remote_srcs = max(n_x - 1, 1)
    vmem = pl.BlockSpec(memory_space=pltpu.VMEM)
    hbm = pl.BlockSpec(memory_space=pl.ANY)
    output = pl.pallas_call(
        functools.partial(kernel, dims),
        out_shape=jax.ShapeDtypeStruct((tok, out_width), BF16),
        in_specs=[hbm] * 7 + [vmem] * 9,
        out_specs=hbm,
        scratch_shapes=[
            pltpu.VMEM((HALO + tok, model), BF16),
            pltpu.VMEM((model, width), BF16),
            pltpu.VMEM((model, width), BF16),
            pltpu.VMEM((n_dp,) + final_projection.shape, BF16),
            pltpu.VMEM((HALO + tok, 2 * gn), F32),
            pltpu.VMEM((HALO + tok, width), F32),
            pltpu.VMEM((tok, gn), BF16),
            pltpu.VMEM((tok, gn), BF16),
            pltpu.VMEM((tok, width), BF16),
            pltpu.VMEM((tok, width), BF16),
            pltpu.VMEM((tok, width), F32),
            pltpu.VMEM((N, width), F32),
            pltpu.VMEM((N, width), BF16),
            pltpu.VMEM((N, width), BF16),
            pltpu.VMEM((tok, width), BF16),
            pltpu.VMEM((tok, out_width), BF16),
            pltpu.VMEM((model, 2 * gn), BF16),
            pltpu.VMEM((increment_projection.shape[1], model), BF16),
            dma((7,)),
            dma,
            dma,
            dma((3, remote_srcs, 3)),
            dma((3, remote_srcs, 3)),
            dma((3, remote_srcs, 3)),
            dma((3, remote_srcs, 3)),
            dma((3, remote_srcs, 2)),
            dma((3, remote_srcs, 2)),
            dma((3, n_x, 4)),
            dma((3, 2)),
            dma((c_chunks,)),
            dma((c_chunks,)),
            dma((n_dp,)),
        ],
        compiler_params=pltpu.CompilerParams(
            collective_id=0, has_side_effects=True, vmem_limit_bytes=56 * 1024 * 1024
        ),
    )(
        hidden,
        source_projection,
        gating_projection,
        final_projection,
        entry_mapping_projection,
        readout_mapping_projection,
        increment_projection.T,
        source_conv_taps,
        entry_mapping_taps,
        readout_mapping_taps,
        increment_offsets[None],
        channel_damping_rate[None],
        bypass_coefficients[None],
        stride_multiplier,
        jnp.swapaxes(added_log_damping, 1, 2),
        norm_scale_factor[None],
    )
    return output[None]


def solution(mesh):
    n_grp, n_sp, n_dp = (mesh.shape[a] for a in ("grp", "sp", "dp"))
    return jax.shard_map(
        functools.partial(shards, (n_grp, n_sp, n_dp, 8)),
        mesh=mesh,
        in_specs=(
            P(("grp", "dp"), "sp", None),
            P("dp", None),
            P("dp", None),
            P(),
            P(),
            P(),
            P(),
            P(),
            P(),
            P(),
            P(),
            P(),
            P(("grp", "dp"), None),
            P(("grp", "dp"), None, None),
            P(),
            P(None, "dp"),
        ),
        out_specs=P(("grp", "dp"), "sp", None),
        check_vma=False,
    )
```
